32 devices in a mesh: ep: 8 (over z, core), tp: 4 (over y, x).
Axes of the slice: x: 2, y: 2, z: 4, core: 2. Of those that a mesh axis runs over, the one named last changes fastest.
Arguments:
- mix_rows: bfloat16 [2048, 2048], P('ep', 'tp'), may hold values from -6 to 6
- mix_gain: bfloat16 [2048], replicated, may hold values from 0.099609375 to 1.8984375
- w_query: bfloat16 [2048, 2048], P(None, 'tp'), may hold values from -0.125 to 0.125
- w_forget: bfloat16 [2048, 2048], P(None, 'tp'), may hold values from -0.125 to 0.125
- w_input: bfloat16 [2048, 2048], P(None, 'tp'), may hold values from -0.125 to 0.125
- w_outgate: bfloat16 [2048, 2048], P(None, 'tp'), may hold values from -0.125 to 0.125
- forget_gap: float32 [2048], P('tp'), may hold values from 1e-05 to 0.1
- decay_extra: float32 [16, 2048], P('tp', 'ep'), may hold values from -0.7 to 0, as said below
- head_gain: bfloat16 [128], replicated, may hold values from 0.099609375 to 1.8984375
- w_mixout: bfloat16 [2048, 2048], P('tp'), may hold values from -0.125 to 0.125
- moe_rows: bfloat16 [2048, 2048], P('ep', 'tp'), may hold values from -6 to 6
- moe_gain: bfloat16 [2048], replicated, may hold values from 0.099609375 to 1.8984375
- route_ids: int32 [2048, 2], P('ep'), may hold values from 0 to 7, all different within a row; in each aligned block of 256 rows (0 to 255, 256 to 511, ...) at most 96 rows name the same one
- route_scores: float32 [2048, 2], P('ep'), may hold values from 0.05 to 1
- w_gate: bfloat16 [8, 2048, 3072], P('ep', None, 'tp'), may hold values from -0.125 to 0.125
- w_up: bfloat16 [8, 2048, 3072], P('ep', None, 'tp'), may hold values from -0.125 to 0.125
- w_down: bfloat16 [8, 3072, 2048], P('ep', 'tp'), may hold values from -0.109375 to 0.109375
Outputs:
- mix_out: bfloat16 [2048, 2048], P('ep', 'tp')
- moe_out: bfloat16 [2048, 2048], P('ep', 'tp')
The draws below stay inside these ranges and needn't reach their ends.
Inputs may be any that keep to these rules, and one draw needn't show every extreme that they name: `route_ids`: each row names 2 different experts. Among the rows of one index of ep at most 96 name the same expert, a bound that at least one block reaches. `decay_extra`: never positive.
All inputs are finite; a program needn't handle non-finite values.
Results may differ from the reference program's by a relative error of at most 0.017.
Values may be sent and summed in bfloat16 or wider, within the bound.
A program may use at most 64 MiB of HBM per device.

```python
import math
import jax
import jax.numpy as jnp
import numpy as np
from jax import lax

HEADS = 16
HEAD_DIM = 128
D = 2048
FFE = 3072
EXPERTS = 8
TOP_K = 2
BLOCK = 64
TOK_A = 256
TOK_B = 256
TOKENS_A = 2048
TOKENS_B = 2048
CAP = 96
N_EP = 8
N_TP = 4


def draw_forget_gap(key, part):
    lowest, highest = (1e-05, 0.1)
    unit = jax.random.uniform(key, (D,), jnp.float32)
    return jnp.exp(jnp.log(lowest) + unit * (jnp.log(highest) - jnp.log(lowest)))


def draw_decay_extra(key, part):
    rate_key, spot_key, depth_key = jax.random.split(key, 3)
    lowest, highest = (1e-05, 0.0001)
    block_list = TOKENS_A // TOK_A
    unit = jax.random.uniform(rate_key, (HEADS, block_list, 1), jnp.float32)
    rate = jnp.exp(jnp.log(lowest) + unit * (jnp.log(highest) - jnp.log(lowest)))
    steady = jnp.broadcast_to(-rate, (HEADS, block_list, TOK_A)).reshape(HEADS, TOKENS_A)
    spots = jax.random.randint(spot_key, (3,), 0, TOKENS_A)
    marked = jnp.any(jnp.arange(TOKENS_A)[None, :] == spots[:, None], axis=0)
    depth = jnp.log(jax.random.uniform(depth_key, (HEADS, TOKENS_A), jnp.float32, 0.5, 0.8))
    return steady + jnp.where(marked[None, :], depth, 0.0)


def block_scale(rng, extent, cuts, smallest, largest):
    factor_of = 1.0
    for position, shards_of in cuts:
        draws = jax.random.uniform(jax.random.fold_in(jax.random.fold_in(rng, 6), position), (shards_of,), jnp.float32, smallest / len(cuts), largest / len(cuts))
        factor_of = factor_of * jnp.repeat(jnp.exp(draws), extent[position] // shards_of).reshape((-1,) + (1,) * (len(extent) - 1 - position))
    return factor_of


def assign_block(key, own, number, rows, amount, top, limit, skew):
    ranking = jax.random.permutation(key, amount)
    crowded, common = load_shares(amount, rows * top, limit, skew, True), load_shares(amount, rows * top, limit, skew, False)
    places = jnp.arange(amount)

    def named(tallies, offset_by):
        used = int((tallies > 0).sum())
        fixed = max(1, used // 4)
        moved = fixed + (places - fixed + offset_by * (used - fixed)) % max(1, amount - fixed)
        return jnp.zeros((amount,), jnp.int32).at[ranking[jnp.where(places < fixed, places, moved)]].set(jnp.asarray(tallies, jnp.int32))

    tallies = jnp.where(number % 4 == 0, named(crowded, number // 4), named(common, number - number // 4 - 1))
    mixed = jax.random.permutation(jax.random.fold_in(own, 3), amount)
    source_of, taker = mixed[0:amount // 2 * 2:2], mixed[1:amount // 2 * 2:2]
    margin = jnp.minimum(tallies[source_of] - 1, limit - tallies[taker]) // 2
    margin = jnp.where((source_of == ranking[0]) | (taker == ranking[0]) | (tallies[taker] == 0), 0, jnp.maximum(margin, 0))
    moved = jax.random.randint(jax.random.fold_in(own, 4), (amount // 2,), 0, 1 << 20) % (margin + 1)
    tallies = tallies.at[source_of].add(-moved).at[taker].add(moved)
    members = jnp.searchsorted(jnp.cumsum(tallies), jnp.arange(rows * top), side="right").astype(jnp.int32)
    table = members.reshape(top, rows).T
    table = table[jax.random.permutation(jax.random.fold_in(own, 1), rows)]
    offset_by = jax.random.randint(jax.random.fold_in(own, 2), (rows, 1), 0, top)
    return jnp.take_along_axis(table, (jnp.arange(top)[None, :] + offset_by) % top, axis=1)


def load_shares(count, total, limit, skew, full):
    portions = [(1 << 20) // math.isqrt(standing ** skew) + 1 for standing in range(1, count + 1)]
    largest = limit if full else min(limit, max(-(-total // count), total * portions[0] // sum(portions)))
    least = 1 if total - largest >= count - 1 else 0
    counts, surplus = [largest] + [least] * (count - 1), total - largest - least * (count - 1)
    while surplus > 0:
        candidates = [i for i in range(1, count) if counts[i] < largest] or [i for i in range(1, count) if counts[i] < limit]
        mass, remaining = sum([portions[i] for i in candidates]), surplus
        for i in candidates:
            addition = min(limit - counts[i], max(1, remaining * portions[i] // mass), surplus)
            counts[i] = counts[i] + addition
            surplus = surplus - addition
    return np.array(counts)


def bell_draw(stream_key, extent, scale, bound, shards=(), held_as=jnp.bfloat16):
    loudness = block_scale(stream_key, extent, shards, -0.22, 0.18) if shards else 1.0
    drawn = jax.random.normal(stream_key, extent, jnp.float32) * scale * loudness
    return jnp.minimum(jnp.maximum(drawn, -bound), bound).astype(held_as)


def setup_inputs(seed: int = 0) -> dict:
    splits = jax.random.split(jax.random.key(seed), 18)
    mix_rows = bell_draw(splits[0], (TOKENS_A, D), 1.0, 6.0, ((0, 8), (1, 4)))
    mix_gain = jnp.clip(1.0 + 0.18 * jax.random.normal(splits[1], (D,), jnp.float32), 0.099609375, 1.8984375).astype(jnp.bfloat16)
    w_query = bell_draw(splits[2], (D, D), D ** -0.5, 0.125, ((1, 4),))
    w_forget = bell_draw(splits[3], (D, D), D ** -0.5, 0.125, ((1, 4),))
    w_input = bell_draw(splits[4], (D, D), D ** -0.5, 0.125, ((1, 4),))
    w_outgate = bell_draw(splits[5], (D, D), D ** -0.5, 0.125, ((1, 4),))
    forget_gap = draw_forget_gap(jax.random.fold_in(splits[17], 71), 0)
    decay_extra = draw_decay_extra(jax.random.fold_in(splits[17], 71), 0)
    head_gain = jnp.clip(1.0 + 0.18 * jax.random.normal(splits[8], (HEAD_DIM,), jnp.float32), 0.099609375, 1.8984375).astype(jnp.bfloat16)
    w_mixout = bell_draw(splits[9], (D, D), D ** -0.5, 0.125, ((0, 4),))
    moe_rows = bell_draw(splits[10], (TOKENS_B, D), 1.0, 6.0, ((0, 8), (1, 4)))
    moe_gain = jnp.clip(1.0 + 0.18 * jax.random.normal(splits[11], (D,), jnp.float32), 0.099609375, 1.8984375).astype(jnp.bfloat16)
    route_ids_keys = jax.random.split(jax.random.fold_in(splits[12], 1), TOKENS_B // TOK_B)
    route_ids_turns = jax.random.permutation(jax.random.fold_in(splits[12], 3), TOKENS_B // TOK_B)
    route_ids = jax.vmap(lambda own, number: assign_block(jax.random.fold_in(splits[12], 2), own, number, TOK_B, EXPERTS, TOP_K, CAP, 1))(route_ids_keys, route_ids_turns).reshape((TOKENS_B, TOP_K))
    route_scores = jnp.clip(0.05 + 0.95 * jax.random.uniform(splits[13], (TOKENS_B, TOP_K), jnp.float32) ** block_scale(splits[13], (TOKENS_B, TOP_K), ((0, 8),), -0.2, 0.2), 0.05, 1.0)
    w_gate = bell_draw(splits[14], (EXPERTS, D, FFE), D ** -0.5, 0.125, ((0, 8), (2, 4)))
    w_up = bell_draw(splits[15], (EXPERTS, D, FFE), D ** -0.5, 0.125, ((0, 8), (2, 4)))
    w_down = bell_draw(splits[16], (EXPERTS, FFE, D), FFE ** -0.5, 0.109375, ((0, 8), (1, 4)))
    return dict(mix_rows=mix_rows, mix_gain=mix_gain, w_query=w_query, w_forget=w_forget, w_input=w_input, w_outgate=w_outgate, forget_gap=forget_gap, decay_extra=decay_extra, head_gain=head_gain, w_mixout=w_mixout, moe_rows=moe_rows, moe_gain=moe_gain, route_ids=route_ids, route_scores=route_scores, w_gate=w_gate, w_up=w_up, w_down=w_down)


epsilon = 1e-06
HIGHEST_PRECISION = lax.Precision.HIGHEST

def rms_scale(rows, gain):
    values = rows.astype(jnp.float32)
    scale = lax.rsqrt(lax.optimization_barrier(jnp.mean(values * values, axis=-1, keepdims=True)) + epsilon)
    return values * scale * gain.astype(jnp.float32)

def block_recurrence(query_rows, key_in, value, log_forget, state):
    heads_count, length, key_dim = query_rows.shape
    block_list = length // BLOCK

    def split(values):
        return jnp.moveaxis(values.reshape(heads_count, block_list, BLOCK, values.shape[2]), 1, 0)
    causal = jnp.tril(jnp.ones((BLOCK, BLOCK), dtype=bool))[:, :, None]

    def advance(carry, inputs):
        query_block, key_block, value_block, forget_block = inputs
        running_state = jnp.cumsum(forget_block, axis=1)
        spread = running_state[:, :, None, :] - running_state[:, None, :, :]
        decay = jnp.exp(jnp.where(causal, spread, -jnp.inf))
        scores = jnp.einsum('hid,hjd,hijd->hij', query_block, key_block, decay, precision=HIGHEST_PRECISION)
        output = jnp.einsum('hid,hde->hie', query_block * jnp.exp(running_state), carry, precision=HIGHEST_PRECISION)
        output = output + jnp.einsum('hij,hje->hie', scores, value_block, precision=HIGHEST_PRECISION)
        last = running_state[:, -1:, :]
        carry = carry * jnp.exp(last)[:, 0, :, None] + jnp.einsum('hjd,hje->hde', key_block * jnp.exp(last - running_state), value_block, precision=HIGHEST_PRECISION)
        return (carry, output)
    carry, outputs = lax.scan(advance, state, (split(query_rows), split(key_in), split(value), split(log_forget)))
    return (jnp.moveaxis(outputs, 0, 1).reshape(heads_count, length, value.shape[2]), carry)

def token_mixer(mix_rows, mix_gain, w_query, w_forget, w_input, w_outgate, forget_gap, decay_extra, head_gain, w_mixout):
    normed = rms_scale(mix_rows, mix_gain).astype(jnp.bfloat16)
    length = normed.shape[0]
    query_preactivation = jnp.dot(normed, w_query, preferred_element_type=jnp.float32)
    forget_pre = jnp.dot(normed, w_forget, preferred_element_type=jnp.float32)
    input_pre = jnp.dot(normed, w_input, preferred_element_type=jnp.float32)
    outgate_pre = jnp.dot(normed, w_outgate, preferred_element_type=jnp.float32)

    def heads(values):
        return values.reshape(length, HEADS, HEAD_DIM).transpose(1, 0, 2)
    query_rows = heads(jax.nn.silu(query_preactivation))
    key_in = heads(forget_gap.astype(jnp.float32) * jax.nn.sigmoid(-forget_pre))
    value = heads(input_pre)
    log_forget = jnp.log1p(-key_in) + decay_extra.astype(jnp.float32)[:, :, None]
    start_state = jnp.zeros((HEADS, HEAD_DIM, HEAD_DIM), jnp.float32)
    head_out, _ = block_recurrence(query_rows, key_in, value, log_forget, start_state)
    gated = rms_scale(head_out, head_gain) * heads(jax.nn.silu(outgate_pre))
    gated = gated.transpose(1, 0, 2).reshape(length, D).astype(jnp.bfloat16)
    group = D // N_TP
    total = jnp.zeros((length, D), jnp.float32)
    for index in range(N_TP):
        part = jnp.dot(gated[:, index * group:(index + 1) * group], w_mixout[index * group:(index + 1) * group], preferred_element_type=jnp.float32)
        total = total + lax.optimization_barrier(part.astype(jnp.bfloat16)).astype(jnp.float32)
    return total.astype(jnp.bfloat16)

def expert_layer(moe_rows, moe_gain, route_ids, route_scores, w_gate, w_up, w_down):
    row_total, top_count = route_ids.shape
    expert_count = w_gate.shape[0]
    normed = rms_scale(moe_rows, moe_gain).astype(jnp.bfloat16)
    weights = route_scores / lax.optimization_barrier(jnp.sum(route_scores, axis=1, keepdims=True))
    grouped = route_ids.reshape(N_EP, TOK_B * top_count).astype(jnp.int32)
    onehot = (grouped[:, :, None] == jnp.arange(expert_count, dtype=jnp.int32)[None, None, :]).astype(jnp.int32)
    rank = lax.optimization_barrier(jnp.sum((jnp.cumsum(onehot, axis=1) - 1) * onehot, axis=2)).astype(jnp.int32)
    source = jnp.arange(N_EP, dtype=jnp.int32)[:, None]
    place = (grouped * (N_EP * CAP) + source * CAP + rank).reshape(-1).astype(jnp.int32)
    token = (jnp.arange(row_total * top_count, dtype=jnp.int32) // top_count).astype(jnp.int32)
    table = jnp.full((expert_count * N_EP * CAP,), row_total, jnp.int32).at[place].set(token)
    padded = jnp.concatenate([normed, jnp.zeros((1, D), jnp.bfloat16)], axis=0)
    slots = padded[table].reshape(expert_count, N_EP * CAP, D)
    width = FFE // N_TP

    def one_expert(operands):
        rows, gate_weight, up_weight, down_weight = operands
        gate_acts = jnp.dot(rows, gate_weight, preferred_element_type=jnp.float32)
        up_acts = jnp.dot(rows, up_weight, preferred_element_type=jnp.float32)
        hidden = (jax.nn.silu(gate_acts) * up_acts).astype(jnp.bfloat16)
        total = jnp.zeros((rows.shape[0], D), jnp.float32)
        for index in range(N_TP):
            part = jnp.dot(hidden[:, index * width:(index + 1) * width], down_weight[index * width:(index + 1) * width], preferred_element_type=jnp.float32)
            total = total + lax.optimization_barrier(part.astype(jnp.bfloat16)).astype(jnp.float32)
        return total.astype(jnp.bfloat16)
    results = lax.map(one_expert, (slots, w_gate, w_up, w_down)).reshape(-1, D)
    picked = results[place].astype(jnp.float32).reshape(row_total, top_count, D)
    return lax.optimization_barrier(jnp.sum(picked * weights[:, :, None], axis=1)).astype(jnp.bfloat16)

def reference(mix_rows, mix_gain, w_query, w_forget, w_input, w_outgate, forget_gap, decay_extra, head_gain, w_mixout, moe_rows, moe_gain, route_ids, route_scores, w_gate, w_up, w_down):
    mix_out = token_mixer(mix_rows, mix_gain, w_query, w_forget, w_input, w_outgate, forget_gap, decay_extra, head_gain, w_mixout)
    moe_out = expert_layer(moe_rows, moe_gain, route_ids, route_scores, w_gate, w_up, w_down)
    return (mix_out, moe_out)
```

```python
import functools

import jax
import jax.numpy as jnp
from jax import lax
from jax.experimental import pallas as pl
from jax.experimental.pallas import tpu as pltpu
from jax.sharding import PartitionSpec as P

BLOCK = 64
epsilon = 1e-06
F32 = jnp.float32
BF16 = jnp.bfloat16
VMEM = pl.BlockSpec(memory_space=pltpu.VMEM)
LIMIT = 60 * 1024 * 1024


def dot(a, b, dims=((1,), (0,)), precision=None):
    return lax.dot_general(a, b, (dims, ((), ())), precision=precision, preferred_element_type=F32)


def sigmoid(x):
    return 1.0 / (1.0 + jnp.exp(-x))


def iota(shape, dim):
    return lax.broadcasted_iota(jnp.int32, shape, dim)


def mixer_kernel(per, x_ref, gain_ref, wq_ref, wf_ref, wi_ref, wo_ref, gap_ref, dec_ref,
                 lo_ref, qd_ref, og_ref, st_ref, normed):
    step = pl.program_id(0)
    length = normed.shape[0]
    dim = st_ref.shape[2]
    parts, _, cols = x_ref.shape

    @pl.when(step == 0)
    def _():
        total = jnp.zeros((length, 1), F32)
        for p in range(parts):
            v = x_ref[p].astype(F32)
            total += jnp.sum(v * v, axis=1, keepdims=True)
        scale = lax.rsqrt(total / (parts * cols) + epsilon)
        for p in range(parts):
            g = gain_ref[:, p * cols:(p + 1) * cols].astype(F32)
            normed[:, p * cols:(p + 1) * cols] = (x_ref[p].astype(F32) * scale * g).astype(BF16)

    n = normed[...]
    qp = dot(n, wq_ref[...])
    fp = dot(n, wf_ref[...])
    value = dot(n, wi_ref[...]).astype(BF16)
    op = dot(n, wo_ref[...])
    query = qp * sigmoid(qp)
    key = gap_ref[...] * sigmoid(-fp)
    og_ref[...] = op * sigmoid(op)
    logs = jnp.log1p(-key)
    dec = dec_ref[...]
    tri = (iota((length, length), 0) >= iota((length, length), 1)).astype(F32)
    causal = iota((BLOCK, BLOCK), 0) >= iota((BLOCK, BLOCK), 1)
    half = BLOCK // 2
    for j in range(per):
        c = slice(j * dim, (j + 1) * dim)
        extra = jnp.sum(jnp.where(iota(dec.shape, 1) == step * per + j, dec, 0.0), axis=1, keepdims=True)
        run = dot(tri, logs[:, c] + extra, precision=lax.Precision.HIGHEST)
        q, k, v = query[:, c], key[:, c], value[:, c]
        qd_ref[:, c] = (q * jnp.exp(run)).astype(BF16)
        state = jnp.zeros((dim, dim), F32)
        base = jnp.zeros((1, dim), F32)
        for b in range(length // BLOCK):
            r = slice(b * BLOCK, (b + 1) * BLOCK)
            g, qb, kb, vb = run[r], q[r], k[r], v[r]
            ref = g[half - 1:half]
            last = g[BLOCK - 1:BLOCK]
            qe = (qb * jnp.exp(g - ref)).astype(BF16)
            ke = (kb * jnp.exp(ref - g)).astype(BF16)
            scores = jnp.where(causal, dot(qe, ke, ((1,), (1,))), 0.0).astype(BF16)
            out = dot(scores, vb)
            if b:
                qs = (qb * jnp.exp(g - base)).astype(BF16)
                out += dot(qs, state.astype(BF16), ((1,), (1,)))
            lo_ref[r, c] = out
            kd = (kb * jnp.exp(last - g)).astype(BF16)
            state = state * jnp.exp(last - base) + dot(vb, kd, ((0,), (0,)))
            base = last
        st_ref[j, 0:dim, :] = state.astype(BF16)
        st_ref[j, dim:, :] = jnp.broadcast_to(jnp.exp(base), (st_ref.shape[1] - dim, dim)).astype(BF16)


def mixer(x, gain, wq, wf, wi, wo, gap, dec):
    parts, length, cols = x.shape
    heads, dim = dec.shape[1], wq.shape[1] // dec.shape[1]
    per = 2 if heads % 2 == 0 else 1
    width = per * dim
    depth = wq.shape[0]
    column = pl.BlockSpec((depth, width), lambda i: (0, i))
    rows = pl.BlockSpec((length, width), lambda i: (0, i))
    whole = lambda s: pl.BlockSpec(s, lambda i: (0,) * len(s))
    return pl.pallas_call(
        functools.partial(mixer_kernel, per),
        grid=(heads // per,),
        in_specs=[whole(x.shape), whole((1, depth)), column, column, column, column,
                  pl.BlockSpec((1, width), lambda i: (0, i)), whole(dec.shape)],
        out_specs=[rows, rows, rows, pl.BlockSpec((per, dim + 16, dim), lambda i: (i, 0, 0))],
        out_shape=[jax.ShapeDtypeStruct((length, heads * dim), F32),
                   jax.ShapeDtypeStruct((length, heads * dim), BF16),
                   jax.ShapeDtypeStruct((length, heads * dim), F32),
                   jax.ShapeDtypeStruct((heads, dim + 16, dim), BF16)],
        scratch_shapes=[pltpu.VMEM((length, depth), BF16)],
        compiler_params=pltpu.CompilerParams(vmem_limit_bytes=LIMIT),
        cost_estimate=pl.CostEstimate(flops=10 * 10**9, bytes_accessed=9 * 10**6, transcendentals=10**6),
    )(x, gain.reshape(1, -1), wq, wf, wi, wo, gap.reshape(1, -1), dec)


def tail_kernel(states_ref, lo_ref, qd_ref, og_ref, hg_ref, w_ref, out_ref, gated):
    place = lax.axis_index("ep")
    hops, heads, _, dim = states_ref.shape
    for h in range(heads):
        c = slice(h * dim, (h + 1) * dim)

        def one(hop, state):
            own = states_ref[hop, h, 0:dim, :].astype(F32)
            passing = states_ref[hop, h, dim:dim + 16, :].astype(F32)[0:1]
            return jnp.where(hop < place, state * passing + own, state)

        state = lax.fori_loop(0, hops, one, jnp.zeros((dim, dim), F32))
        out = lo_ref[:, c] + dot(qd_ref[:, c], state.astype(BF16), ((1,), (1,)))
        scale = lax.rsqrt(jnp.mean(out * out, axis=1, keepdims=True) + epsilon)
        gated[:, c] = (out * scale * hg_ref[...].astype(F32) * og_ref[:, c]).astype(BF16)
    parts, _, cols = out_ref.shape
    for p in range(parts):
        out_ref[p] = dot(gated[...], w_ref[:, p * cols:(p + 1) * cols]).astype(BF16)


def tail(states, lo, qd, og, hg, w, parts):
    length, width = lo.shape
    return pl.pallas_call(
        tail_kernel,
        in_specs=[VMEM] * 6,
        out_specs=VMEM,
        out_shape=jax.ShapeDtypeStruct((parts, length, w.shape[1] // parts), BF16),
        scratch_shapes=[pltpu.VMEM((length, width), BF16)],
        compiler_params=pltpu.CompilerParams(vmem_limit_bytes=LIMIT),
        cost_estimate=pl.CostEstimate(flops=10**9, bytes_accessed=5 * 10**6, transcendentals=10**5),
    )(states, lo, qd, og, hg.reshape(1, -1), w)


def ranks(ids, experts):
    tokens = ids.shape[1]
    names = iota((experts, tokens), 0)
    picks = [names == ids[k:k + 1, :] for k in range(ids.shape[0])]
    chosen = functools.reduce(jnp.logical_or, picks)
    before = (iota((tokens, tokens), 0) < iota((tokens, tokens), 1)).astype(BF16)
    return picks, chosen, dot(chosen.astype(BF16), before)


def slot_hits(mask, rank, experts, capacity):
    rows = experts * capacity
    owner = iota((rows, experts), 0) - iota((rows, experts), 1) * capacity
    owner = jnp.logical_and(owner >= 0, owner < capacity).astype(F32)
    tokens = rank.shape[1]
    spread = dot(owner, jnp.where(mask, rank, -1.0))
    spot = dot(owner, iota((experts, tokens), 0).astype(F32)) * capacity
    return (spread >= 0.0) & (spread + spot == iota((rows, tokens), 0).astype(F32))


def dispatch_kernel(experts, capacity, ids_ref, rows_ref, out_ref):
    _, chosen, rank = ranks(ids_ref[...], experts)
    hits = slot_hits(chosen, rank, experts, capacity).astype(BF16)
    out_ref[...] = dot(hits, rows_ref[...]).astype(BF16)


def dispatch(ids, rows, experts, capacity):
    return pl.pallas_call(
        functools.partial(dispatch_kernel, experts, capacity),
        in_specs=[VMEM] * 2,
        out_specs=VMEM,
        out_shape=jax.ShapeDtypeStruct((experts * capacity, rows.shape[1]), BF16),
    )(ids, rows)


def combine_kernel(experts, capacity, ids_ref, scores_ref, back_ref, out_ref):
    picks, _, rank = ranks(ids_ref[...], experts)
    scores = scores_ref[...]
    weights = scores / jnp.sum(scores, axis=1, keepdims=True)
    total = jnp.zeros(out_ref.shape, F32)
    for k, mask in enumerate(picks):
        hits = slot_hits(mask, rank, experts, capacity).astype(BF16)
        total += dot(hits, back_ref[...], ((0,), (0,))) * weights[:, k:k + 1]
    out_ref[...] = total.astype(BF16)


def combine(ids, scores, back, experts, capacity):
    return pl.pallas_call(
        functools.partial(combine_kernel, experts, capacity),
        in_specs=[VMEM] * 3,
        out_specs=VMEM,
        out_shape=jax.ShapeDtypeStruct((ids.shape[1], back.shape[1]), BF16),
    )(ids, scores, back)


def expert_kernel(x_ref, gain_ref, wg_ref, wu_ref, wd_ref, out_ref, normed, total):
    step = pl.program_id(0)
    parts, rows, cols = x_ref.shape

    @pl.when(step == 0)
    def _():
        squares = jnp.zeros((rows, 1), F32)
        for p in range(parts):
            v = x_ref[p].astype(F32)
            squares += jnp.sum(v * v, axis=1, keepdims=True)
        scale = lax.rsqrt(squares / (parts * cols) + epsilon)
        for p in range(parts):
            g = gain_ref[:, p * cols:(p + 1) * cols].astype(F32)
            normed[:, p * cols:(p + 1) * cols] = (x_ref[p].astype(F32) * scale * g).astype(BF16)

    gate = dot(normed[...], wg_ref[0])
    up = dot(normed[...], wu_ref[0])
    hidden = (gate * sigmoid(gate) * up).astype(BF16)
    last = pl.num_programs(0) - 1
    for p in range(parts):
        c = slice(p * cols, (p + 1) * cols)
        part = dot(hidden, wd_ref[0, :, c])

        @pl.when(jnp.logical_and(step == 0, last > 0))
        def _():
            total[:, c] = part

        @pl.when(jnp.logical_and(step > 0, step < last))
        def _():
            total[:, c] += part

        @pl.when(step == last)
        def _():
            out_ref[p] = (jnp.where(step > 0, total[:, c], 0.0) + part).astype(BF16)


def experts_call(x, gain, wg, wu, wd):
    parts, rows, cols = x.shape
    depth, units = wg.shape[1:]
    tile = 256 if units % 256 == 0 else units
    return pl.pallas_call(
        expert_kernel,
        grid=(units // tile,),
        in_specs=[pl.BlockSpec(x.shape, lambda i: (0, 0, 0)), pl.BlockSpec((1, depth), lambda i: (0, 0)),
                  pl.BlockSpec((1, depth, tile), lambda i: (0, 0, i)),
                  pl.BlockSpec((1, depth, tile), lambda i: (0, 0, i)),
                  pl.BlockSpec((1, tile, depth), lambda i: (0, i, 0))],
        out_specs=pl.BlockSpec(x.shape, lambda i: (0, 0, 0)),
        out_shape=jax.ShapeDtypeStruct(x.shape, BF16),
        scratch_shapes=[pltpu.VMEM((rows, depth), BF16), pltpu.VMEM((rows, depth), F32)],
        compiler_params=pltpu.CompilerParams(vmem_limit_bytes=LIMIT),
        cost_estimate=pl.CostEstimate(flops=8 * 10**9, bytes_accessed=10**7, transcendentals=10**6),
    )(x, gain.reshape(1, -1), wg, wu, wd)


def per_device(mix_rows, mix_gain, w_query, w_forget, w_input, w_outgate, forget_gap, decay_extra,
               head_gain, w_mixout, moe_rows, moe_gain, route_ids, route_scores, w_gate, w_up, w_down):
    eps, tps = lax.axis_size("ep"), lax.axis_size("tp")
    tokens, top = route_ids.shape
    experts = w_gate.shape[0] * eps
    capacity = tokens * top * 3 // (2 * experts)
    cols = mix_rows.shape[1]
    ids = route_ids.T
    slots = dispatch(ids, moe_rows, experts, capacity)
    arrived = lax.all_to_all(slots.reshape(eps, -1, cols), "ep", split_axis=0, concat_axis=0, tiled=True)
    gathered = lax.all_gather(arrived.reshape(-1, cols), "tp", axis=0)
    mix_whole = lax.all_gather(mix_rows, "tp", axis=0)
    lo, qd, og, st = mixer(mix_whole, mix_gain, w_query, w_forget, w_input, w_outgate, forget_gap, decay_extra.T)
    product = experts_call(gathered, moe_gain, w_gate, w_up, w_down)
    expert_sum = lax.psum_scatter(product, "tp", scatter_dimension=0)
    states = lax.all_gather(st, "ep", axis=0)
    mixed = tail(states, lo, qd, og, head_gain, w_mixout, tps)
    mix_out = lax.psum_scatter(mixed, "tp", scatter_dimension=0)
    back = lax.all_to_all(expert_sum.reshape(eps, -1, cols), "ep", split_axis=0, concat_axis=0, tiled=True)
    moe_out = combine(ids, route_scores, back.reshape(-1, cols), experts, capacity)
    return (mix_out, moe_out)


def solution(mesh):
    placed = (
        P("ep", "tp"), P(), P(None, "tp"), P(None, "tp"), P(None, "tp"), P(None, "tp"), P("tp"),
        P("tp", "ep"), P(), P("tp", None), P("ep", "tp"), P(), P("ep", None), P("ep", None),
        P("ep", None, "tp"), P("ep", None, "tp"), P("ep", "tp", None),
    )
    return jax.shard_map(
        per_device, mesh=mesh, in_specs=placed,
        out_specs=(P("ep", "tp"), P("ep", "tp")), check_vma=False,
    )
```
